32 devices in a mesh: fs: 4 (over z), rep: 4 (over y, x), tp: 2 (over core).
Axes of the slice: x: 2, y: 2, z: 4, core: 2. Of those that a mesh axis runs over, the one named last changes fastest.
Arguments:
- saved_input: bfloat16 [16384, 2048], P(('fs', 'rep')), may hold values from -6 to 6
- value_cotangent: bfloat16 [16384, 4096], P(('fs', 'rep'), 'tp'), may hold values from -0.0061950684 to 0.0061950684
- factor: bfloat16 [2048, 128], P('fs'), may hold values from -1.5 to 1.5
- weight: float32 [2048, 4096], P('fs', 'tp'), may hold values from -1.2 to 1.2
- first_moment: float32 [128, 4096], P('fs', 'tp'), may hold values from -1.8 to 1.8
- second_moment: float32 [128, 4096], P('fs', 'tp'), may hold values from 0.1 to 1
Outputs:
- low_grad: float32 [128, 4096], P('fs', 'tp')
- new_first: float32 [128, 4096], P('fs', 'tp')
- new_second: float32 [128, 4096], P('fs', 'tp')
- direction: float32 [2048, 4096], P('fs', 'tp')
- new_weight: float32 [2048, 4096], P('fs', 'tp')
- new_copy: bfloat16 [2048, 4096], P('fs', 'tp')
The draws below stay inside these ranges and needn't reach their ends.
All inputs are finite; a program needn't handle non-finite values.
Results may differ from the reference program's by a relative error of at most 0.006.
Values may be sent and summed in bfloat16 or wider, within the bound.
A program may use at most 64 MiB of HBM per device.

```python
import math
import jax
import jax.numpy as jnp
from jax import lax

D = 2048
E = 4096
R = 128
TOKENS = 16384


def with_spikes(entries, key, source, target, shards_of, factor):
    owner, partner = [(jnp.arange(entries.shape[axis_at]) // (entries.shape[axis_at] // shards_of)).reshape([-1 if axis == axis_at else 1 for axis in range(entries.ndim)]) for axis_at in (source, target)]
    chosen = jax.random.permutation(key, shards_of)[partner]
    strong = (owner == chosen) | (owner == (partner + shards_of // 2) % shards_of)
    return jnp.where(strong, factor * entries, entries)


def steps_of(own_key, shape, pieces, least, top_value):
    gain = 1.0
    for dim, shards_of in pieces:
        draws = jax.random.uniform(jax.random.fold_in(jax.random.fold_in(own_key, 6), dim), (shards_of,), jnp.float32, least / len(pieces), top_value / len(pieces))
        gain = gain * jnp.repeat(jnp.exp(draws), shape[dim] // shards_of).reshape((-1,) + (1,) * (len(shape) - 1 - dim))
    return gain


def gaussian(rng, shape, scale, most, cuts=(), kind=jnp.bfloat16):
    drawn = jax.random.normal(rng, shape, jnp.float32) * scale
    if len(cuts) > 0:
        drawn = steps_of(rng, shape, cuts, -0.22, 0.18) * drawn
    return jnp.clip(drawn, min=-most, max=most).astype(kind)


def heavy_noise(rng, extent, scale, limit, cuts, heavy, kind=jnp.bfloat16):
    entries = scale * jax.random.normal(rng, extent, jnp.float32)
    if cuts:
        entries = entries * steps_of(rng, extent, cuts, -0.22, 0.18)
    return jnp.clip(with_spikes(entries, jax.random.fold_in(rng, 3), *heavy), -limit, limit).astype(kind)


def setup_inputs(seed: int = 0) -> dict:
    key_of = jax.random.split(jax.random.key(seed), 7)
    saved_input = heavy_noise(key_of[0], (TOKENS, D), 1.0, 6.0, ((0, 16),), (0, 1, 16, 2.0))
    value_cotangent = gaussian(key_of[1], (TOKENS, E), (6.0 / (D * TOKENS) ** 0.5), 0.0061950684, ((0, 16), (1, 2)))
    factor = gaussian(key_of[2], (D, R), 0.25, 1.5, ((0, 4),))
    weight = gaussian(key_of[3], (D, E), 0.2, 1.2, ((0, 4), (1, 2)), jnp.float32)
    first_moment = gaussian(key_of[4], (R, E), 0.3, 1.8, ((0, 4), (1, 2)), jnp.float32)
    second_moment = jnp.clip(jnp.exp(math.log(1.0) - 2.3025851 * jax.random.uniform(key_of[5], (R, E), jnp.float32) ** steps_of(key_of[5], (R, E), ((0, 4), (1, 2)), -0.2, 0.2)), 0.1, 1.0)
    return dict(saved_input=saved_input, value_cotangent=value_cotangent, factor=factor, weight=weight, first_moment=first_moment, second_moment=second_moment)


first_decay = 0.9
second_decay = 0.9
learn_rate = 0.05
epsilon = 1e-08

def reference(saved_input, value_cotangent, factor, weight, first_moment, second_moment):
    grad = lax.dot_general(saved_input, value_cotangent, (((0,), (0,)), ((), ())), preferred_element_type=jnp.float32)
    factor_wide = factor.astype(jnp.float32)
    low_grad = lax.dot_general(factor_wide, grad, (((0,), (0,)), ((), ())), precision=lax.Precision.HIGHEST)
    new_first = first_decay * first_moment + (1.0 - first_decay) * low_grad
    new_second = second_decay * second_moment + (1.0 - second_decay) * low_grad * low_grad
    ratio = new_first / (jnp.sqrt(new_second) + epsilon)
    raw = jnp.dot(factor_wide, ratio, precision=lax.Precision.HIGHEST)
    spread = jnp.sqrt(jnp.sum(raw * raw) / (D * E))
    direction = raw / (spread + 1.0)
    new_weight = weight - learn_rate * direction
    return (low_grad, new_first, new_second, direction, new_weight, new_weight.astype(jnp.bfloat16))
```

```python
import functools

import jax
import jax.numpy as jnp
from jax import lax
from jax.experimental import pallas as pl
from jax.experimental.pallas import tpu as pltpu
from jax.sharding import PartitionSpec as P

first_decay = 0.9
second_decay = 0.9
learn_rate = 0.05
epsilon = 1e-08

CHUNKS = 2
TILE = 64
MESH = pl.DeviceIdType.MESH


def moved(src, dst, send, recv, where):
    return pltpu.make_async_remote_copy(
        src_ref=src, dst_ref=dst, send_sem=send, recv_sem=recv, device_id=where, device_id_type=MESH
    )


def merged(ref, count, rows):
    if rows % 16 == 0:
        block = ref[...]
        return block.reshape(count * rows, block.shape[-1])
    pieces = [ref[i].astype(jnp.float32) for i in range(count)]
    return jnp.concatenate(pieces, axis=0).astype(jnp.bfloat16)


def exchange(
    nfs, nrep, ntp, entries,
    x_hbm, v_hbm, f_hbm, m1_hbm, m2_hbm,
    ratio_out, low_out, scale_out,
    x, v, m1, m2, fall, proj, pt, gram,
    own1, send1, recv1, own2, send2, recv2, low_own, low_all, rgat, rall, sc_send, sc_recv,
    local_sem, fs_send, fs_recv, fd_send, fd_recv, s1_send, s1_recv, s2_send, s2_recv,
    a1_send, a1_recv, a2_send, a2_recv, lg_send, lg_recv, t_send, t_recv,
):
    f, r, c = lax.axis_index("fs"), lax.axis_index("rep"), lax.axis_index("tp")
    hr = fall.shape[2]
    rank, cw = own1.shape[1], own1.shape[2]
    block = cw * CHUNKS
    rp = rank // nfs
    f32, bf16 = jnp.float32, jnp.bfloat16

    locals_ = [
        pltpu.make_async_copy(f_hbm.at[pl.ds(0, hr)], fall.at[f, 0], local_sem.at[0]),
        pltpu.make_async_copy(f_hbm.at[pl.ds(hr, hr)], fall.at[f, 1], local_sem.at[1]),
        pltpu.make_async_copy(x_hbm, x, local_sem.at[2]),
        pltpu.make_async_copy(v_hbm, v, local_sem.at[3]),
        pltpu.make_async_copy(m1_hbm, m1, local_sem.at[4]),
        pltpu.make_async_copy(m2_hbm, m2, local_sem.at[5]),
    ]
    for copy in locals_:
        copy.start()

    barrier = pltpu.get_barrier_semaphore()
    for e in range(1, nfs):
        pl.semaphore_signal(barrier, inc=1, device_id={"fs": lax.rem(f + e, nfs)}, device_id_type=MESH)
    for d in range(1, nrep):
        pl.semaphore_signal(barrier, inc=1, device_id={"rep": lax.rem(r + d, nrep)}, device_id_type=MESH)
    other = {"tp": 1 - c}
    pl.semaphore_signal(barrier, inc=1, device_id=other, device_id_type=MESH)
    pl.semaphore_wait(barrier, nfs + nrep - 1)

    sends = []

    fcopies, dcopies = [], []
    for e in range(1, nfs):
        copy = moved(
            f_hbm.at[pl.ds(c * hr, hr)], fall.at[f, c], fs_send.at[e - 1], fs_recv.at[e - 1],
            {"fs": lax.rem(f + e, nfs)},
        )
        copy.start()
        fcopies.append(copy)
        sends.append(copy)
    incremental = (2 * hr) % 128 == 0

    def project(src, first):
        piece = fall[src].reshape(2 * hr, fall.shape[3])
        cols = pl.ds(pl.multiple_of(src * (2 * hr), 128), 2 * hr)
        term = jnp.dot(x[:, cols], piece, preferred_element_type=f32)
        if first:
            proj[...] = term
        else:
            proj[...] += term

    locals_[0].wait()
    locals_[1].wait()
    locals_[2].wait()
    if incremental:
        project(f, True)
    for e in range(1, nfs + 1):
        if e < nfs:
            src = lax.rem(f - e + nfs, nfs)
            fcopies[e - 1].wait_recv()
            copy = moved(fall.at[src, c], fall.at[src, c], fd_send.at[e - 1], fd_recv.at[e - 1], other)
            copy.start()
            dcopies.append(copy)
            sends.append(copy)
        if e > 1:
            dcopies[e - 2].wait_recv()
            if incremental:
                project(lax.rem(f - (e - 1) + nfs, nfs), False)
    if not incremental:
        whole = fall[...].reshape(nfs * 2 * hr, fall.shape[3])
        proj[...] = jnp.dot(x[...], whole, preferred_element_type=f32)

    turned = proj[...].T
    upper = turned.astype(bf16)
    pt[:rank] = upper
    pt[rank:] = (turned - upper.astype(f32)).astype(bf16)

    locals_[3].wait()
    copies1 = {}
    for q in range(CHUNKS):
        for d in list(range(1, nrep)) + [0]:
            to = lax.rem(r + d, nrep)
            cols = pl.ds(pl.multiple_of(to * block + q * cw, 128), cw)
            both = jnp.dot(pt[...], v[:, cols], preferred_element_type=f32)
            term = both[:rank] + both[rank:]
            if d == 0:
                own1[q] = term
            else:
                send1[q, d - 1] = term.astype(bf16)
                copy = moved(
                    send1.at[q, d - 1], recv1.at[q, d - 1], s1_send.at[q, d - 1], s1_recv.at[q, d - 1],
                    {"rep": to},
                )
                copy.start()
                copies1[q, d] = copy
                sends.append(copy)

    whole = fall[...].reshape(nfs * 2 * hr, fall.shape[3])
    square = lax.dot_general(whole, whole, (((0,), (0,)), ((), ())), preferred_element_type=f32)
    upper = square.astype(bf16)
    gram[:rank] = upper
    gram[rank:] = (square - upper.astype(f32)).astype(bf16)
    locals_[4].wait()
    locals_[5].wait()

    copies2 = {}
    for q in range(CHUNKS):
        total = own1[q]
        for d in range(1, nrep):
            copies1[q, d].wait_recv()
            total = total + recv1[q, d - 1].astype(f32)
        for i in range(nfs):
            part = total[i * rp:(i + 1) * rp]
            own2[q, i] = part
            send2[q, i] = part.astype(bf16)
        for e in range(1, nfs):
            to = lax.rem(f + e, nfs)
            copy = moved(
                send2.at[q, to], recv2.at[q, e - 1], s2_send.at[q, e - 1], s2_recv.at[q, e - 1], {"fs": to}
            )
            copy.start()
            copies2[q, e] = copy
            sends.append(copy)

    copies3, low_copies = {}, []
    for q in range(CHUNKS):
        low = own2[q, f]
        for e in range(1, nfs):
            copies2[q, e].wait_recv()
            low = low + recv2[q, e - 1].astype(f32)
        cols = pl.ds(pl.multiple_of(r * block + q * cw, 128), cw)
        new_first = first_decay * m1[:, cols] + (1.0 - first_decay) * low
        new_second = second_decay * m2[:, cols] + (1.0 - second_decay) * low * low
        ratio = new_first / (jnp.sqrt(new_second) + epsilon)
        rgat[q, f] = ratio.astype(bf16)
        low_own[q] = low
        for e in range(1, nfs):
            copy = moved(
                rgat.at[q, f], rgat.at[q, f], a1_send.at[q, e - 1], a1_recv.at[q, e - 1],
                {"fs": lax.rem(f + e, nfs)},
            )
            copy.start()
            copies3[q, e] = copy
            sends.append(copy)
        for d in range(1, nrep):
            copy = moved(
                low_own.at[q], low_all.at[q, d - 1], lg_send.at[q, d - 1], lg_recv.at[q, d - 1],
                {"rep": lax.rem(r + d, nrep)},
            )
            copy.start()
            low_copies.append((q, d, copy))
            sends.append(copy)

    squares = jnp.zeros((1, 1), f32)

    def place(piece, owner, q):
        cols = pl.ds(pl.multiple_of(owner * block + q * cw, 128), cw)
        ratio_out[:, cols] = piece
        both = jnp.dot(gram[...], piece, preferred_element_type=f32)
        terms = (both[:rank] + both[rank:]) * piece.astype(f32)
        return jnp.sum(jnp.sum(terms, axis=0, keepdims=True), axis=1, keepdims=True)

    copies4 = {}
    for q in range(CHUNKS):
        for e in range(1, nfs):
            copies3[q, e].wait_recv()
        for d in range(1, nrep):
            copy = moved(
                rgat.at[q], rall.at[q, d - 1], a2_send.at[q, d - 1], a2_recv.at[q, d - 1],
                {"rep": lax.rem(r + d, nrep)},
            )
            copy.start()
            copies4[q, d] = copy
            sends.append(copy)
        squares = squares + place(merged(rgat.at[q], nfs, rp), r, q)
        cols = pl.ds(pl.multiple_of(r * block + q * cw, 128), cw)
        low_out[:, cols] = low_own[q]

    for q, d, copy in low_copies:
        copy.wait_recv()
        owner = lax.rem(r - d + nrep, nrep)
        low_out[:, pl.ds(pl.multiple_of(owner * block + q * cw, 128), cw)] = low_all[q, d - 1]

    for q in range(CHUNKS):
        for d in range(1, nrep):
            copies4[q, d].wait_recv()
            piece = merged(rall.at[q, d - 1], nfs, rp)
            squares = squares + place(piece, lax.rem(r - d + nrep, nrep), q)

    sc_send[...] = jnp.broadcast_to(squares, sc_send.shape)
    copy = moved(sc_send, sc_recv, t_send, t_recv, other)
    copy.start()
    sends.append(copy)
    copy.wait_recv()
    spread = jnp.sqrt((sc_send[...] + sc_recv[...]) / entries)
    scale_out[...] = 1.0 / (spread + 1.0)
    for copy in sends:
        copy.wait_send()


def update(factor, ratio, scale, low, m1, m2, weight, low_out, first_out, second_out, dir_out, weight_out, copy_out):
    @pl.when(pl.program_id(0) == 0)
    def _():
        grad = low[...]
        low_out[...] = grad
        first_out[...] = first_decay * m1[...] + (1.0 - first_decay) * grad
        second_out[...] = second_decay * m2[...] + (1.0 - second_decay) * grad * grad

    raw = jnp.dot(factor[...], ratio[...], preferred_element_type=jnp.float32)
    direction = raw * scale[0:1, 0:1]
    dir_out[...] = direction
    new_weight = weight[...] - learn_rate * direction
    weight_out[...] = new_weight
    copy_out[...] = new_weight.astype(jnp.bfloat16)


def on_device(nfs, nrep, ntp, saved_input, value_cotangent, factor, weight, first_moment, second_moment):
    f32, bf16 = jnp.float32, jnp.bfloat16
    tokens, width = saved_input.shape
    cols = value_cotangent.shape[1]
    rows, rank = factor.shape
    rp = rank // nfs
    cw = cols // nrep // CHUNKS
    hr = rows // 2
    any_spec = pl.BlockSpec(memory_space=pl.ANY)
    vmem = pl.BlockSpec(memory_space=pltpu.VMEM)
    dma = pltpu.SemaphoreType.DMA
    V = pltpu.VMEM
    pf, pr = nfs - 1, nrep - 1
    ratio, low, scale = pl.pallas_call(
        functools.partial(exchange, nfs, nrep, ntp, float(width) * cols * ntp),
        out_shape=(
            jax.ShapeDtypeStruct((rank, cols), bf16),
            jax.ShapeDtypeStruct((rp, cols), f32),
            jax.ShapeDtypeStruct((8, 128), f32),
        ),
        in_specs=[any_spec] * 5,
        out_specs=(vmem, vmem, vmem),
        scratch_shapes=[
            V((tokens, width), bf16),
            V((tokens, cols), bf16),
            V((rp, cols), f32),
            V((rp, cols), f32),
            V((nfs, 2, hr, rank), bf16),
            V((tokens, rank), f32),
            V((2 * rank, tokens), bf16),
            V((2 * rank, rank), bf16),
            V((CHUNKS, rank, cw), f32),
            V((CHUNKS, pr, rank, cw), bf16),
            V((CHUNKS, pr, rank, cw), bf16),
            V((CHUNKS, nfs, rp, cw), f32),
            V((CHUNKS, nfs, rp, cw), bf16),
            V((CHUNKS, pf, rp, cw), bf16),
            V((CHUNKS, rp, cw), f32),
            V((CHUNKS, pr, rp, cw), f32),
            V((CHUNKS, nfs, rp, cw), bf16),
            V((CHUNKS, pr, nfs, rp, cw), bf16),
            V((8, 128), f32),
            V((8, 128), f32),
            dma((6,)),
            dma((pf,)), dma((pf,)), dma((pf,)), dma((pf,)),
            dma((CHUNKS, pr)), dma((CHUNKS, pr)),
            dma((CHUNKS, pf)), dma((CHUNKS, pf)),
            dma((CHUNKS, pf)), dma((CHUNKS, pf)),
            dma((CHUNKS, pr)), dma((CHUNKS, pr)),
            dma((CHUNKS, pr)), dma((CHUNKS, pr)),
            dma, dma,
        ],
        compiler_params=pltpu.CompilerParams(
            collective_id=0, has_side_effects=True, vmem_limit_bytes=40 * 1024 * 1024
        ),
        name="exchange",
    )(saved_input, value_cotangent, factor, first_moment, second_moment)

    tile = min(TILE, rows)
    fixed = lambda shape: pl.BlockSpec(shape, lambda i: (0, 0))
    moving = lambda shape: pl.BlockSpec(shape, lambda i: (i, 0))
    return pl.pallas_call(
        update,
        grid=(rows // tile,),
        out_shape=(
            jax.ShapeDtypeStruct((rp, cols), f32),
            jax.ShapeDtypeStruct((rp, cols), f32),
            jax.ShapeDtypeStruct((rp, cols), f32),
            jax.ShapeDtypeStruct((rows, cols), f32),
            jax.ShapeDtypeStruct((rows, cols), f32),
            jax.ShapeDtypeStruct((rows, cols), bf16),
        ),
        in_specs=[
            moving((tile, rank)),
            fixed((rank, cols)),
            fixed((8, 128)),
            fixed((rp, cols)),
            fixed((rp, cols)),
            fixed((rp, cols)),
            moving((tile, cols)),
        ],
        out_specs=(
            fixed((rp, cols)), fixed((rp, cols)), fixed((rp, cols)),
            moving((tile, cols)), moving((tile, cols)), moving((tile, cols)),
        ),
        name="update",
    )(factor, ratio, scale, low, first_moment, second_moment, weight)


def solution(mesh):
    placed = (
        P(("fs", "rep"), None),
        P(("fs", "rep"), "tp"),
        P("fs", None),
        P("fs", "tp"),
        P("fs", "tp"),
        P("fs", "tp"),
    )
    sizes = mesh.shape
    return jax.shard_map(
        functools.partial(on_device, sizes["fs"], sizes["rep"], sizes["tp"]),
        mesh=mesh,
        in_specs=placed,
        out_specs=(P("fs", "tp"),) * 6,
        check_vma=False,
    )
```
